32 devices in a mesh: rep: 2 (over x), fs: 8 (over z, y), tp: 2 (over core).
Axes of the slice: x: 2, y: 2, z: 4, core: 2. Of those that a mesh axis runs over, the one named last changes fastest.
Arguments:
- tokens: bfloat16 [8192, 2048], P(('rep', 'fs', 'tp')), may hold values from -6 to 6
- norm_gain: float32 [2048], replicated, may hold values from 0.1 to 1.9
- gate_weight: float32 [2048, 5120], P('fs', 'tp'), may hold values from -0.125 to 0.125
- gate_scale: float32 [5120], P('tp'), may hold values from 0.1 to 1.9
- up_weight: float32 [2048, 5120], P('fs', 'tp'), may hold values from -0.125 to 0.125
- up_scale: float32 [5120], P('tp'), may hold values from 0.1 to 1.9
- down_weight: float32 [5120, 2048], P('tp', 'fs'), may hold values from -0.078125 to 0.078125
- down_scale: float32 [2048], replicated, may hold values from 0.1 to 1.9
Outputs:
- mixed: bfloat16 [8192, 2048], P(('rep', 'fs', 'tp'))
The draws below stay inside these ranges and needn't reach their ends.
All inputs are finite; a program needn't handle non-finite values.
Results may differ from the reference program's by a relative error of at most 0.013.
Values may be sent and summed in bfloat16 or wider, within the bound.
A program may use at most 128 MiB of HBM per device.

```python
import jax
import jax.numpy as jnp
from jax import lax

D = 2048
FF = 5120
TOK_DEV = 256
TOKENS = 8192
N_TP = 2


def steps_of(key, shape, cuts, low, top_value):
    def one(position, blocks):
        steps = jax.random.uniform(jax.random.fold_in(jax.random.fold_in(key, 6), position), (blocks,), jnp.float32, low / len(cuts), top_value / len(cuts))
        return jnp.repeat(jnp.exp(steps), shape[position] // blocks).reshape((-1,) + (1,) * (len(shape) - position - 1))

    level = one(*cuts[0])
    for cut in cuts[1:]:
        level = level * one(*cut)
    return level


def bell_draw(key, extent, spread, limit, pieces=(), kind=jnp.bfloat16):
    drawn = spread * jax.random.normal(key, extent, jnp.float32)
    if pieces:
        drawn = drawn * steps_of(key, extent, pieces, -0.22, 0.18)
    return jnp.clip(drawn, -limit, limit).astype(kind)


def setup_inputs(seed: int = 0) -> dict:
    splits = jax.random.split(jax.random.key(seed), 9)
    return {
        "tokens": bell_draw(splits[0], (TOKENS, D), 1.0, 6.0, ((0, 32),)),
        "norm_gain": jnp.clip(1.0 + 0.18 * jax.random.normal(splits[1], (D,), jnp.float32), 0.1, 1.9),
        "gate_weight": bell_draw(splits[2], (D, FF), D ** -0.5, 0.125, ((0, 8), (1, 2)), jnp.float32),
        "gate_scale": jnp.clip(1.0 + 0.18 * jax.random.normal(splits[3], (FF,), jnp.float32), 0.1, 1.9),
        "up_weight": bell_draw(splits[4], (D, FF), D ** -0.5, 0.125, ((0, 8), (1, 2)), jnp.float32),
        "up_scale": jnp.clip(1.0 + 0.18 * jax.random.normal(splits[5], (FF,), jnp.float32), 0.1, 1.9),
        "down_weight": bell_draw(splits[6], (FF, D), FF ** -0.5, 0.078125, ((0, 2), (1, 8)), jnp.float32),
        "down_scale": jnp.clip(1.0 + 0.18 * jax.random.normal(splits[7], (D,), jnp.float32), 0.1, 1.9),
    }


EPS_VALUE = 1e-06

def normalize(token_rows, norm_gain):
    values = token_rows.astype(jnp.float32)
    inverse = lax.rsqrt(lax.optimization_barrier(jnp.mean(values * values, axis=-1, keepdims=True)) + EPS_VALUE)
    return (values * inverse * norm_gain).astype(jnp.bfloat16)

def reference(tokens, norm_gain, gate_weight, gate_scale, up_weight, up_scale, down_weight, down_scale):
    gate_bf = gate_weight.astype(jnp.bfloat16)
    up_bf = up_weight.astype(jnp.bfloat16)
    down_bf = down_weight.astype(jnp.bfloat16)
    width_tp = FF // N_TP
    down_blocks = down_bf.reshape(N_TP, width_tp, D)
    group_rows = TOK_DEV * N_TP

    def one_group(token_rows):
        normed = normalize(token_rows, norm_gain)
        gate_pre = jnp.dot(normed, gate_bf, preferred_element_type=jnp.float32) * gate_scale
        up_pre = jnp.dot(normed, up_bf, preferred_element_type=jnp.float32) * up_scale
        hidden = (jax.nn.silu(gate_pre) * up_pre).astype(jnp.bfloat16)
        total = jnp.zeros((group_rows, D), jnp.float32)
        for tp_block in range(N_TP):
            columns = hidden[:, tp_block * width_tp:(tp_block + 1) * width_tp]
            partial_value = (jnp.dot(columns, down_blocks[tp_block], preferred_element_type=jnp.float32) * down_scale).astype(jnp.bfloat16)
            partial_value = lax.optimization_barrier(partial_value)
            total = total + partial_value.astype(jnp.float32)
        return total.astype(jnp.bfloat16)
    grouped = tokens.reshape(TOKENS // group_rows, group_rows, D)
    return lax.map(one_group, grouped).reshape(TOKENS, D)
```

```python
import functools

import jax
import jax.numpy as jnp
from jax import lax
from jax.experimental import pallas as pl
from jax.experimental.pallas import tpu as pltpu
from jax.sharding import PartitionSpec as P

EPS_VALUE = 1e-06


def from_partner(shard, axis, distance):
    return lax.ppermute(shard, axis, [(i, i ^ 1 << distance) for i in range(lax.axis_size(axis))])


def normalize(token_rows, norm_gain):
    values = token_rows.astype(jnp.float32)
    inverse = lax.rsqrt(jnp.mean(values * values, axis=-1, keepdims=True) + EPS_VALUE)
    return (values * inverse * norm_gain).astype(jnp.bfloat16)


def body(tokens, norm_gain, gate_weight, gate_scale, up_weight, up_scale, down_weight, down_scale):
    normed = normalize(tokens, norm_gain)
    gate_bf = gate_weight.astype(jnp.bfloat16)
    up_bf = up_weight.astype(jnp.bfloat16)
    down_bf = down_weight.astype(jnp.bfloat16)
    rep_index = lax.axis_index("rep")
    half_cols = gate_bf.shape[1] // 2
    half_rows = down_bf.shape[0] // 2
    own_gate = lax.dynamic_slice_in_dim(gate_bf, rep_index * half_cols, half_cols, 1)
    own_up = lax.dynamic_slice_in_dim(up_bf, rep_index * half_cols, half_cols, 1)
    own_down = lax.dynamic_slice_in_dim(down_bf, rep_index * half_rows, half_rows, 0)
    own_parts = (
        lax.all_gather(own_gate, "fs", axis=0, tiled=True),
        lax.all_gather(own_up, "fs", axis=0, tiled=True),
        lax.all_gather(own_down, "fs", axis=1, tiled=True),
    )
    far_parts = from_partner((own_parts[0], own_parts[1], own_parts[2]), "rep", 0)
    is_first = rep_index == 0

    def joined(own_part, far_part, axis_dim):
        return jnp.where(
            is_first,
            jnp.concatenate([own_part, far_part], axis_dim),
            jnp.concatenate([far_part, own_part], axis_dim),
        )

    gate_full = joined(own_parts[0], far_parts[0], 1)
    up_full = joined(own_parts[1], far_parts[1], 1)
    down_full = joined(own_parts[2], far_parts[2], 0)
    slab_rows = lax.all_gather(normed, "tp", axis=0, tiled=True)
    gate_pre = jnp.dot(slab_rows, gate_full, preferred_element_type=jnp.float32) * gate_scale
    up_pre = jnp.dot(slab_rows, up_full, preferred_element_type=jnp.float32) * up_scale
    hidden = (jax.nn.silu(gate_pre) * up_pre).astype(jnp.bfloat16)
    partial_value = (
        jnp.dot(hidden, down_full, preferred_element_type=jnp.float32) * down_scale
    ).astype(jnp.bfloat16)
    partial_value = lax.optimization_barrier(partial_value)
    return lax.psum_scatter(
        partial_value.astype(jnp.float32).astype(jnp.bfloat16),
        "tp",
        scatter_dimension=0,
        tiled=True,
    )


MESH = pl.DeviceIdType.MESH


def ffn_kernel(
    sizes, tok_ref, gain_ref, gate_ref, gscale_ref, up_ref, uscale_ref, down_ref, dscale_ref, out_ref,
    wg, wu, wd, rows_x, acc_g, acc_u, hid, staged, landed,
    copy_sem, ring_send, ring_recv, down_send, down_recv, tok_send, tok_recv, part_send, part_recv,
):
    n_rep, n_fs, n_tp = sizes
    group = n_rep * n_tp
    steps = n_fs - 1
    half_ring = n_fs // 2
    n_tok, width = tok_ref.shape
    depth = wg.shape[1]
    half_depth = depth // 2
    cols = wd.shape[3]
    half_hid = wd.shape[2] // 2

    rep = lax.axis_index("rep")
    fs = lax.axis_index("fs")
    tp = lax.axis_index("tp")
    member = rep * n_tp + tp

    side = fs % 2
    place = (1 - side) * (fs // 2) + side * (n_fs - 1 - fs // 2)

    def fs_at(position):
        spot = (position + 2 * n_fs) % n_fs
        back = spot // half_ring
        return (1 - back) * 2 * spot + back * (2 * (n_fs - 1 - spot) + 1)

    right = (rep, fs_at(place + 1), tp)
    left = (rep, fs_at(place - 1), tp)

    def peer(offset):
        other = (member + offset) % group
        return other, (other // n_tp, fs, other % n_tp)

    def origin(direction, hops):
        return fs_at(place - hops) if direction == 0 else fs_at(place + hops)

    def ring_copy(direction, piece, step):
        store = wg if direction == 0 else wu
        part = store.at[origin(direction, step), pl.ds(piece * half_depth, half_depth)]
        return pltpu.make_async_remote_copy(
            src_ref=part, dst_ref=part,
            send_sem=ring_send.at[direction, piece, step], recv_sem=ring_recv.at[direction, piece, step],
            device_id=right if direction == 0 else left, device_id_type=MESH,
        )

    def ring_arrival(direction, piece, step):
        store = wg if direction == 0 else wu
        part = store.at[origin(direction, step + 1), pl.ds(piece * half_depth, half_depth)]
        return pltpu.make_async_remote_copy(
            src_ref=part, dst_ref=part,
            send_sem=ring_send.at[direction, piece, step], recv_sem=ring_recv.at[direction, piece, step],
            device_id=right if direction == 0 else left, device_id_type=MESH,
        )

    def down_copy(direction, piece, step, hops):
        part = wd.at[origin(direction, hops), direction, pl.ds(piece * half_hid, half_hid)]
        return pltpu.make_async_remote_copy(
            src_ref=part, dst_ref=part,
            send_sem=down_send.at[direction, piece, step], recv_sem=down_recv.at[direction, piece, step],
            device_id=right if direction == 0 else left, device_id_type=MESH,
        )

    def token_copy(offset, slot):
        return pltpu.make_async_remote_copy(
            src_ref=rows_x.at[slot], dst_ref=rows_x.at[slot],
            send_sem=tok_send.at[offset - 1], recv_sem=tok_recv.at[offset - 1],
            device_id=peer(offset)[1], device_id_type=MESH,
        )

    def part_copy(offset, index):
        other, where = peer(offset)
        return pltpu.make_async_remote_copy(
            src_ref=staged.at[index, other], dst_ref=landed.at[index, offset - 1],
            send_sem=part_send.at[index, offset - 1], recv_sem=part_recv.at[index, offset - 1],
            device_id=where, device_id_type=MESH,
        )

    own = [
        pltpu.make_async_copy(gate_ref, wg.at[fs], copy_sem.at[0]),
        pltpu.make_async_copy(up_ref, wu.at[fs], copy_sem.at[1]),
        pltpu.make_async_copy(down_ref.at[:, pl.ds(0, cols)], wd.at[fs, 0], copy_sem.at[2]),
        pltpu.make_async_copy(down_ref.at[:, pl.ds(cols, cols)], wd.at[fs, 1], copy_sem.at[3]),
    ]
    for copy in own:
        copy.start()
    barrier = pltpu.get_barrier_semaphore()
    for device in [right, left] + [peer(offset)[1] for offset in range(1, group)]:
        pl.semaphore_signal(barrier, inc=1, device_id=device, device_id_type=MESH)
    pl.semaphore_wait(barrier, group + 1)
    own[0].wait()
    own[1].wait()
    for piece in range(2):
        for direction in range(2):
            ring_copy(direction, piece, 0).start()

    values = tok_ref[...].astype(jnp.float32)
    inverse = lax.rsqrt(jnp.mean(values * values, axis=-1, keepdims=True) + EPS_VALUE)
    rows_x[member] = (values * inverse * gain_ref[...]).astype(jnp.bfloat16)
    own[2].wait()
    own[3].wait()
    for offset in range(1, group):
        token_copy(offset, member).start()

    def add_slice(index):
        gate_fs, up_fs = origin(0, index), origin(1, index)
        gate_cols = pl.ds(pl.multiple_of(gate_fs * depth, depth), depth)
        up_cols = pl.ds(pl.multiple_of(up_fs * depth, depth), depth)

        def tile(block, carry):
            gate_term = jnp.dot(rows_x[block, :, gate_cols], wg[gate_fs], preferred_element_type=jnp.float32)
            up_term = jnp.dot(rows_x[block, :, up_cols], wu[up_fs], preferred_element_type=jnp.float32)

            @pl.when(index == 0)
            def _():
                acc_g[block] = gate_term
                acc_u[block] = up_term

            @pl.when(index > 0)
            def _():
                acc_g[block] += gate_term
                acc_u[block] += up_term

            return carry

        lax.fori_loop(0, group, tile, 0)

    def ring_step(step, carry):
        for piece in range(2):
            for direction in range(2):
                ring_arrival(direction, piece, step).wait_recv()

                @pl.when(step < steps - 1)
                def _():
                    ring_copy(direction, piece, step + 1).start()

        @pl.when(step == steps - 3)
        def _():
            for piece in range(2):
                for direction in range(2):
                    down_copy(direction, piece, 0, 0).start()

        @pl.when(step == half_ring - 1)
        def _():
            for offset in range(1, group):
                token_copy(offset, (member + group - offset) % group).wait_recv()

        @pl.when(step == steps - 1)
        def _():
            for piece in range(2):
                for direction in range(2):
                    down_copy(direction, piece, 0, 1).wait_recv()
                    down_copy(direction, piece, 1, 1).start()

        @pl.when(step >= half_ring - 1)
        def _():
            first = 2 * (step - (half_ring - 1))

            def one(extra, inner):
                add_slice(first + extra)
                return inner

            lax.fori_loop(0, 2, one, 0)

        return carry

    lax.fori_loop(0, steps, ring_step, 0)

    def activate(block, carry):
        gate_pre = acc_g[block] * gscale_ref[...]
        up_pre = acc_u[block] * uscale_ref[...]
        hid[block] = (jax.nn.silu(gate_pre) * up_pre).astype(jnp.bfloat16)
        return carry

    lax.fori_loop(0, group, activate, 0)

    def produce(hops):
        for direction in range(2):
            source = origin(direction, hops)
            start = pl.multiple_of(source * 2 * cols + direction * cols, cols)
            scale = dscale_ref[:, pl.ds(start, cols)]
            index = 2 * hops + direction

            def tile(block, carry):
                product = jnp.dot(hid[block], wd[source, direction], preferred_element_type=jnp.float32)
                staged[index, block] = (product * scale).astype(jnp.bfloat16)
                return carry

            lax.fori_loop(0, group, tile, 0)
            for offset in range(1, group):
                part_copy(offset, index).start()

    def down_step(step, carry):
        @pl.when((step >= 2) & (step <= steps))
        def _():
            for piece in range(2):
                for direction in range(2):
                    down_copy(direction, piece, step - 1, step).wait_recv()

                    @pl.when(step < steps)
                    def _():
                        down_copy(direction, piece, step, step).start()

        produce(step)
        return carry

    lax.fori_loop(0, n_fs, down_step, 0)

    def finish(hops, carry):
        for direction in range(2):
            index = 2 * hops + direction
            total = staged[index, member].astype(jnp.float32)
            for offset in range(1, group):
                part_copy(offset, index).wait_recv()
                total = total + landed[index, offset - 1].astype(jnp.float32)
            start = pl.multiple_of(origin(direction, hops) * 2 * cols + direction * cols, cols)
            out_ref[:, pl.ds(start, cols)] = total.astype(out_ref.dtype)
        return carry

    lax.fori_loop(0, n_fs, finish, 0)

    def drain(step, carry):
        for piece in range(2):
            for direction in range(2):
                ring_copy(direction, piece, step).wait_send()
                down_copy(direction, piece, step, step).wait_send()
        return carry

    lax.fori_loop(0, steps, drain, 0)

    def drain_parts(index, carry):
        for offset in range(1, group):
            part_copy(offset, index).wait_send()
        return carry

    lax.fori_loop(0, 2 * n_fs, drain_parts, 0)
    for offset in range(1, group):
        token_copy(offset, member).wait_send()


def kernel_body(sizes, tokens, norm_gain, gate_weight, gate_scale, up_weight, up_scale, down_weight, down_scale):
    n_rep, n_fs, n_tp = sizes
    group = n_rep * n_tp
    n_tok, width = tokens.shape
    depth = gate_weight.shape[0]
    units = gate_weight.shape[1] // n_rep
    cols = down_weight.shape[1] // 2
    first = lax.axis_index("rep") * units
    own_gate = lax.dynamic_slice_in_dim(gate_weight, first, units, 1).astype(jnp.bfloat16)
    own_up = lax.dynamic_slice_in_dim(up_weight, first, units, 1).astype(jnp.bfloat16)
    own_down = lax.dynamic_slice_in_dim(down_weight, first, units, 0).astype(jnp.bfloat16)
    own_gate_scale = lax.dynamic_slice_in_dim(gate_scale, first, units, 0)
    own_up_scale = lax.dynamic_slice_in_dim(up_scale, first, units, 0)
    vmem = pl.BlockSpec(memory_space=pltpu.VMEM)
    anywhere = pl.BlockSpec(memory_space=pl.ANY)
    steps = n_fs - 1
    bf = jnp.bfloat16
    dma = pltpu.SemaphoreType.DMA
    return pl.pallas_call(
        functools.partial(ffn_kernel, sizes),
        out_shape=jax.ShapeDtypeStruct((n_tok, width), bf),
        in_specs=[vmem, vmem, anywhere, vmem, anywhere, vmem, anywhere, vmem],
        out_specs=vmem,
        scratch_shapes=[
            pltpu.VMEM((n_fs, depth, units), bf),
            pltpu.VMEM((n_fs, depth, units), bf),
            pltpu.VMEM((n_fs, 2, units, cols), bf),
            pltpu.VMEM((group, n_tok, width), bf),
            pltpu.VMEM((group, n_tok, units), jnp.float32),
            pltpu.VMEM((group, n_tok, units), jnp.float32),
            pltpu.VMEM((group, n_tok, units), bf),
            pltpu.VMEM((2 * n_fs, group, n_tok, cols), bf),
            pltpu.VMEM((2 * n_fs, group - 1, n_tok, cols), bf),
            dma((4,)),
            dma((2, 2, steps)), dma((2, 2, steps)),
            dma((2, 2, steps)), dma((2, 2, steps)),
            dma((group - 1,)), dma((group - 1,)),
            dma((2 * n_fs, group - 1)), dma((2 * n_fs, group - 1)),
        ],
        compiler_params=pltpu.CompilerParams(
            collective_id=0, has_side_effects=True, vmem_limit_bytes=62 * 1024 * 1024
        ),
    )(
        tokens, norm_gain[None, :], own_gate, own_gate_scale[None, :], own_up, own_up_scale[None, :],
        own_down, down_scale[None, :],
    )


def fits_kernel(mesh, tokens, gate_weight, down_weight):
    n_rep, n_fs, n_tp = (mesh.shape[name] for name in ("rep", "fs", "tp"))
    units = gate_weight.shape[1] // (n_tp * n_rep)
    aligned = units % 128 == 0 and down_weight.shape[1] // n_fs % 256 == 0
    return aligned and n_fs % 2 == 0 and n_fs >= 8 and n_rep * n_tp <= 4


def solution(mesh):
    sizes = tuple(mesh.shape[name] for name in ("rep", "fs", "tp"))

    def run(tokens, norm_gain, gate_weight, gate_scale, up_weight, up_scale, down_weight, down_scale):
        chosen = body
        if fits_kernel(mesh, tokens, gate_weight, down_weight):
            chosen = functools.partial(kernel_body, sizes)
        return jax.shard_map(
            chosen,
            mesh=mesh,
            in_specs=(
                P(("rep", "fs", "tp"), None),
                P(),
                P("fs", "tp"),
                P("tp"),
                P("fs", "tp"),
                P("tp"),
                P("tp", "fs"),
                P(),
            ),
            out_specs=P(("rep", "fs", "tp"), None),
            check_vma=False,
        )(tokens, norm_gain, gate_weight, gate_scale, up_weight, up_scale, down_weight, down_scale)

    return run
```

```python
import functools

import jax
import jax.numpy as jnp
from jax import lax
from jax.experimental import pallas as pl
from jax.experimental.pallas import tpu as pltpu
from jax.sharding import PartitionSpec as P

EPS_VALUE = 1e-06


def from_partner(shard, axis, distance):
    return lax.ppermute(shard, axis, [(i, i ^ 1 << distance) for i in range(lax.axis_size(axis))])


def normalize(token_rows, norm_gain):
    values = token_rows.astype(jnp.float32)
    inverse = lax.rsqrt(jnp.mean(values * values, axis=-1, keepdims=True) + EPS_VALUE)
    return (values * inverse * norm_gain).astype(jnp.bfloat16)


def body(tokens, norm_gain, gate_weight, gate_scale, up_weight, up_scale, down_weight, down_scale):
    normed = normalize(tokens, norm_gain)
    gate_bf = gate_weight.astype(jnp.bfloat16)
    up_bf = up_weight.astype(jnp.bfloat16)
    down_bf = down_weight.astype(jnp.bfloat16)
    rep_index = lax.axis_index("rep")
    half_cols = gate_bf.shape[1] // 2
    half_rows = down_bf.shape[0] // 2
    own_gate = lax.dynamic_slice_in_dim(gate_bf, rep_index * half_cols, half_cols, 1)
    own_up = lax.dynamic_slice_in_dim(up_bf, rep_index * half_cols, half_cols, 1)
    own_down = lax.dynamic_slice_in_dim(down_bf, rep_index * half_rows, half_rows, 0)
    own_parts = (
        lax.all_gather(own_gate, "fs", axis=0, tiled=True),
        lax.all_gather(own_up, "fs", axis=0, tiled=True),
        lax.all_gather(own_down, "fs", axis=1, tiled=True),
    )
    far_parts = from_partner((own_parts[0], own_parts[1], own_parts[2]), "rep", 0)
    is_first = rep_index == 0

    def joined(own_part, far_part, axis_dim):
        return jnp.where(
            is_first,
            jnp.concatenate([own_part, far_part], axis_dim),
            jnp.concatenate([far_part, own_part], axis_dim),
        )

    gate_full = joined(own_parts[0], far_parts[0], 1)
    up_full = joined(own_parts[1], far_parts[1], 1)
    down_full = joined(own_parts[2], far_parts[2], 0)
    slab_rows = lax.all_gather(normed, "tp", axis=0, tiled=True)
    gate_pre = jnp.dot(slab_rows, gate_full, preferred_element_type=jnp.float32) * gate_scale
    up_pre = jnp.dot(slab_rows, up_full, preferred_element_type=jnp.float32) * up_scale
    hidden = (jax.nn.silu(gate_pre) * up_pre).astype(jnp.bfloat16)
    partial_value = (
        jnp.dot(hidden, down_full, preferred_element_type=jnp.float32) * down_scale
    ).astype(jnp.bfloat16)
    partial_value = lax.optimization_barrier(partial_value)
    return lax.psum_scatter(
        partial_value.astype(jnp.float32).astype(jnp.bfloat16),
        "tp",
        scatter_dimension=0,
        tiled=True,
    )


MESH = pl.DeviceIdType.MESH


def ffn_kernel(
    sizes, tok_ref, gain_ref, gate_ref, gscale_ref, up_ref, uscale_ref, down_ref, dscale_ref, out_ref,
    raw_g, raw_u, raw_d, wg, wu, wd, rows_x, acc_g, acc_u, hid, staged, landed,
    copy_sem, ring_send, ring_recv, down_send, down_recv, tok_send, tok_recv, part_send, part_recv,
):
    n_rep, n_fs, n_tp = sizes
    group = n_rep * n_tp
    steps = n_fs - 1
    half_ring = n_fs // 2
    n_tok, width = tok_ref.shape
    depth = wg.shape[1]
    half_depth = depth // 2
    cols = wd.shape[3]
    half_hid = wd.shape[2] // 2

    rep = lax.axis_index("rep")
    fs = lax.axis_index("fs")
    tp = lax.axis_index("tp")
    member = rep * n_tp + tp

    side = fs % 2
    place = (1 - side) * (fs // 2) + side * (n_fs - 1 - fs // 2)

    def fs_at(position):
        spot = (position + 2 * n_fs) % n_fs
        back = spot // half_ring
        return (1 - back) * 2 * spot + back * (2 * (n_fs - 1 - spot) + 1)

    right = (rep, fs_at(place + 1), tp)
    left = (rep, fs_at(place - 1), tp)

    def peer(offset):
        other = (member + offset) % group
        return other, (other // n_tp, fs, other % n_tp)

    def origin(direction, hops):
        return fs_at(place - hops) if direction == 0 else fs_at(place + hops)

    def ring_copy(direction, piece, step):
        store = wg if direction == 0 else wu
        part = store.at[origin(direction, step), pl.ds(piece * half_depth, half_depth)]
        return pltpu.make_async_remote_copy(
            src_ref=part, dst_ref=part,
            send_sem=ring_send.at[direction, piece, step], recv_sem=ring_recv.at[direction, piece, step],
            device_id=right if direction == 0 else left, device_id_type=MESH,
        )

    def ring_arrival(direction, piece, step):
        store = wg if direction == 0 else wu
        part = store.at[origin(direction, step + 1), pl.ds(piece * half_depth, half_depth)]
        return pltpu.make_async_remote_copy(
            src_ref=part, dst_ref=part,
            send_sem=ring_send.at[direction, piece, step], recv_sem=ring_recv.at[direction, piece, step],
            device_id=right if direction == 0 else left, device_id_type=MESH,
        )

    def down_copy(direction, piece, step, hops):
        part = wd.at[origin(direction, hops), direction, pl.ds(piece * half_hid, half_hid)]
        return pltpu.make_async_remote_copy(
            src_ref=part, dst_ref=part,
            send_sem=down_send.at[direction, piece, step], recv_sem=down_recv.at[direction, piece, step],
            device_id=right if direction == 0 else left, device_id_type=MESH,
        )

    def token_copy(offset, slot):
        return pltpu.make_async_remote_copy(
            src_ref=rows_x.at[slot], dst_ref=rows_x.at[slot],
            send_sem=tok_send.at[offset - 1], recv_sem=tok_recv.at[offset - 1],
            device_id=peer(offset)[1], device_id_type=MESH,
        )

    def part_copy(offset, index):
        other, where = peer(offset)
        return pltpu.make_async_remote_copy(
            src_ref=staged.at[index, other], dst_ref=landed.at[index, offset - 1],
            send_sem=part_send.at[index, offset - 1], recv_sem=part_recv.at[index, offset - 1],
            device_id=where, device_id_type=MESH,
        )

    units = pl.ds(pl.multiple_of(rep * wg.shape[2], 128), wg.shape[2])
    loads = []
    for piece in range(2):
        part = pl.ds(piece * half_depth, half_depth)
        for direction, source, store in ((0, gate_ref, raw_g), (1, up_ref, raw_u)):
            loads.append(
                pltpu.make_async_copy(source.at[part, units], store.at[part], copy_sem.at[2 * piece + direction])
            )
    loads.append(pltpu.make_async_copy(down_ref.at[units], raw_d, copy_sem.at[4]))
    for load in loads:
        load.start()
    barrier = pltpu.get_barrier_semaphore()
    for device in [right, left] + [peer(offset)[1] for offset in range(1, group)]:
        pl.semaphore_signal(barrier, inc=1, device_id=device, device_id_type=MESH)

    def round_piece(direction, piece):
        loads[2 * piece + direction].wait()
        part = slice(piece * half_depth, (piece + 1) * half_depth)
        raw, store = (raw_g, wg) if direction == 0 else (raw_u, wu)
        store[fs, part] = raw[part].astype(jnp.bfloat16)

    round_piece(0, 0)
    round_piece(1, 0)
    pl.semaphore_wait(barrier, group + 1)
    ring_copy(0, 0, 0).start()
    round_piece(0, 1)
    ring_copy(1, 0, 0).start()
    round_piece(1, 1)
    ring_copy(0, 1, 0).start()

    values = tok_ref[...].astype(jnp.float32)
    inverse = lax.rsqrt(jnp.mean(values * values, axis=-1, keepdims=True) + EPS_VALUE)
    rows_x[member] = (values * inverse * gain_ref[...]).astype(jnp.bfloat16)
    ring_copy(1, 1, 0).start()
    loads[4].wait()
    for direction in range(2):
        wd[fs, direction] = raw_d[:, direction * cols:(direction + 1) * cols].astype(jnp.bfloat16)
    for offset in range(1, group):
        token_copy(offset, member).start()

    def add_slice(index):
        gate_fs, up_fs = origin(0, index), origin(1, index)
        gate_cols = pl.ds(pl.multiple_of(gate_fs * depth, depth), depth)
        up_cols = pl.ds(pl.multiple_of(up_fs * depth, depth), depth)

        def tile(block, carry):
            gate_term = jnp.dot(rows_x[block, :, gate_cols], wg[gate_fs], preferred_element_type=jnp.float32)
            up_term = jnp.dot(rows_x[block, :, up_cols], wu[up_fs], preferred_element_type=jnp.float32)

            @pl.when(index == 0)
            def _():
                acc_g[block] = gate_term
                acc_u[block] = up_term

            @pl.when(index > 0)
            def _():
                acc_g[block] += gate_term
                acc_u[block] += up_term

            return carry

        lax.fori_loop(0, group, tile, 0)

    def ring_step(step, carry):
        @pl.when(step == steps - 3)
        def _():
            for piece in range(2):
                for direction in range(2):
                    down_copy(direction, piece, 0, 0).start()

        def both(piece, inner):
            for direction in range(2):
                ring_arrival(direction, piece, step).wait_recv()

                @pl.when(step < steps - 1)
                def _():
                    ring_copy(direction, piece, step + 1).start()

            @pl.when(step == steps - 1)
            def _():
                for direction in range(2):
                    down_copy(direction, piece, 0, 1).wait_recv()
                    down_copy(direction, piece, 1, 1).start()

            @pl.when((step == half_ring - 1) & (piece == 0))
            def _():
                for offset in range(1, group):
                    token_copy(offset, (member + group - offset) % group).wait_recv()

            @pl.when(step >= half_ring - 1)
            def _():
                add_slice(2 * (step - (half_ring - 1)) + piece)

            return inner

        return lax.fori_loop(0, 2, both, carry)

    lax.fori_loop(0, steps, ring_step, 0)

    def activate(block, carry):
        gate_pre = acc_g[block] * gscale_ref[:, units]
        up_pre = acc_u[block] * uscale_ref[:, units]
        hid[block] = (jax.nn.silu(gate_pre) * up_pre).astype(jnp.bfloat16)
        return carry

    lax.fori_loop(0, group, activate, 0)

    def produce(hops):
        for direction in range(2):
            source = origin(direction, hops)
            start = pl.multiple_of(source * 2 * cols + direction * cols, cols)
            scale = dscale_ref[:, pl.ds(start, cols)]
            index = 2 * hops + direction

            def tile(turn, carry):
                block = (member + 1 + turn) % group
                product = jnp.dot(hid[block], wd[source, direction], preferred_element_type=jnp.float32)
                staged[index, block] = (product * scale).astype(jnp.bfloat16)
                return carry

            lax.fori_loop(0, group, tile, 0)
            for offset in range(1, group):
                part_copy(offset, index).start()

    def down_step(step, carry):
        hops = step + 2
        for piece in range(2):
            for direction in range(2):
                down_copy(direction, piece, hops - 1, hops).wait_recv()

                @pl.when(hops < steps)
                def _():
                    down_copy(direction, piece, hops, hops).start()

        low = step + 2 * ((step // 2 + n_fs - 1) // n_fs)
        high = step + 1 + 2 * ((step + n_fs - 1) // n_fs)

        def one(done_hops, inner):
            produce(done_hops)
            return inner

        return lax.fori_loop(low, high, one, carry)

    lax.fori_loop(0, n_fs - 2, down_step, 0)

    def finish(hops, carry):
        for direction in range(2):
            index = 2 * hops + direction
            total = staged[index, member].astype(jnp.float32)
            for offset in range(1, group):
                part_copy(offset, index).wait_recv()
                total = total + landed[index, offset - 1].astype(jnp.float32)
            start = pl.multiple_of(origin(direction, hops) * 2 * cols + direction * cols, cols)
            out_ref[:, pl.ds(start, cols)] = total.astype(out_ref.dtype)
        return carry

    lax.fori_loop(0, n_fs, finish, 0)

    def drain(step, carry):
        for piece in range(2):
            for direction in range(2):
                ring_copy(direction, piece, step).wait_send()
                down_copy(direction, piece, step, step).wait_send()
        return carry

    lax.fori_loop(0, steps, drain, 0)

    def drain_parts(index, carry):
        for offset in range(1, group):
            part_copy(offset, index).wait_send()
        return carry

    lax.fori_loop(0, 2 * n_fs, drain_parts, 0)
    for offset in range(1, group):
        token_copy(offset, member).wait_send()


def kernel_body(sizes, tokens, norm_gain, gate_weight, gate_scale, up_weight, up_scale, down_weight, down_scale):
    n_rep, n_fs, n_tp = sizes
    group = n_rep * n_tp
    n_tok, width = tokens.shape
    depth = gate_weight.shape[0]
    units = gate_weight.shape[1] // n_rep
    cols = down_weight.shape[1] // 2
    vmem = pl.BlockSpec(memory_space=pltpu.VMEM)
    anywhere = pl.BlockSpec(memory_space=pl.ANY)
    steps = n_fs - 1
    bf = jnp.bfloat16
    dma = pltpu.SemaphoreType.DMA
    return pl.pallas_call(
        functools.partial(ffn_kernel, sizes),
        out_shape=jax.ShapeDtypeStruct((n_tok, width), bf),
        in_specs=[vmem, vmem, anywhere, vmem, anywhere, vmem, anywhere, vmem],
        out_specs=vmem,
        scratch_shapes=[
            pltpu.VMEM((depth, units), jnp.float32),
            pltpu.VMEM((depth, units), jnp.float32),
            pltpu.VMEM((units, 2 * cols), jnp.float32),
            pltpu.VMEM((n_fs, depth, units), bf),
            pltpu.VMEM((n_fs, depth, units), bf),
            pltpu.VMEM((n_fs, 2, units, cols), bf),
            pltpu.VMEM((group, n_tok, width), bf),
            pltpu.VMEM((group, n_tok, units), jnp.float32),
            pltpu.VMEM((group, n_tok, units), jnp.float32),
            pltpu.VMEM((group, n_tok, units), bf),
            pltpu.VMEM((2 * n_fs, group, n_tok, cols), bf),
            pltpu.VMEM((2 * n_fs, group - 1, n_tok, cols), bf),
            dma((5,)),
            dma((2, 2, steps)), dma((2, 2, steps)),
            dma((2, 2, steps)), dma((2, 2, steps)),
            dma((group - 1,)), dma((group - 1,)),
            dma((2 * n_fs, group - 1)), dma((2 * n_fs, group - 1)),
        ],
        compiler_params=pltpu.CompilerParams(
            collective_id=0, has_side_effects=True, vmem_limit_bytes=62 * 1024 * 1024
        ),
    )(
        tokens, norm_gain[None, :], gate_weight, gate_scale[None, :], up_weight, up_scale[None, :],
        down_weight, down_scale[None, :],
    )


def fits_kernel(mesh, tokens, gate_weight, down_weight):
    n_rep, n_fs, n_tp = (mesh.shape[name] for name in ("rep", "fs", "tp"))
    units = gate_weight.shape[1] // (n_tp * n_rep)
    aligned = units % 128 == 0 and down_weight.shape[1] // n_fs % 256 == 0
    return aligned and n_fs % 2 == 0 and n_fs >= 8 and n_rep * n_tp <= 4


def solution(mesh):
    sizes = tuple(mesh.shape[name] for name in ("rep", "fs", "tp"))

    def run(tokens, norm_gain, gate_weight, gate_scale, up_weight, up_scale, down_weight, down_scale):
        chosen = body
        if fits_kernel(mesh, tokens, gate_weight, down_weight):
            chosen = functools.partial(kernel_body, sizes)
        return jax.shard_map(
            chosen,
            mesh=mesh,
            in_specs=(
                P(("rep", "fs", "tp"), None),
                P(),
                P("fs", "tp"),
                P("tp"),
                P("fs", "tp"),
                P("tp"),
                P("tp", "fs"),
                P(),
            ),
            out_specs=P(("rep", "fs", "tp"), None),
            check_vma=False,
        )(tokens, norm_gain, gate_weight, gate_scale, up_weight, up_scale, down_weight, down_scale)

    return run
```
